256 devices in a mesh: ep: 16 (over y, x), tp: 16 (over z, core).
Axes of the slice: x: 4, y: 4, z: 8, core: 2. Of those that a mesh axis runs over, the one named last changes fastest.
Arguments:
- scan_source_values: bfloat16 [1024, 32768], P('tp', 'ep'), may hold values from -6 to 6
- switch_path_values: bfloat16 [1024, 32768], P('tp', 'ep'), may hold values from -6 to 6
- causal_filter_coefficients: bfloat16 [1024, 4], replicated, may hold values from -3 to 3
- scan_switch_blockmap: bfloat16 [16, 64, 64], replicated, may hold values from -0.75 to 0.75
- entry_switch_blockmap: bfloat16 [16, 64, 64], replicated, may hold values from -0.75 to 0.75
- feature_fading_speeds: float32 [1024], replicated, may hold values from 0 to 1
- spike_amount: float32 [32768], P('ep'), may hold values from -1 to 0
- final_linear_map: bfloat16 [1024, 2048], replicated, may hold values from -0.1875 to 0.1875
- dispatched_group_activity: bfloat16 [32768, 2048], P(('ep', 'tp')), may hold values from -6 to 6
- specialist_rmsgain: bfloat16 [2048], replicated, may hold values from 0.099609375 to 1.8984375
- selected_specialist_ids: int32 [32768, 2], P(('ep', 'tp')), may hold values from 0 to 15, all different within a row; in each aligned block of 128 rows (0 to 127, 128 to 255, ...) at most 24 rows name the same one
- selected_specialist_share: float32 [32768, 2], P(('ep', 'tp')), may hold values from 0.2 to 1
- specialist_switch_maps: bfloat16 [16, 2048, 2048], P('ep', None, 'tp'), may hold values from -0.3125 to 0.3125
- specialist_widen_maps: bfloat16 [16, 2048, 2048], P('ep', None, 'tp'), may hold values from -0.3125 to 0.3125
- specialist_shrink_maps: bfloat16 [16, 2048, 2048], P('ep', None, 'tp'), may hold values from -0.03125 to 0.03125
Outputs:
- scan_path_result: bfloat16 [32768, 2048], P(('ep', 'tp'))
- moe_out: bfloat16 [32768, 2048], P(('ep', 'tp'))
The draws below stay inside these ranges and needn't reach their ends.
Inputs may be any that keep to these rules, and one draw needn't show every extreme that they name: `selected_specialist_ids`: each row names 2 different experts. Among the rows of one device no expert is named more than 24 times, and in every draw some device names some expert exactly 24 times.
All inputs are finite; a program needn't handle non-finite values.
Results may differ from the reference program's by a relative error of at most 0.0085.
Values may be sent and summed in bfloat16 or wider, within the bound.
No kernel may reach another device: no remote copies, remote signals or barrier semaphores. Data moves between devices by JAX's collectives and lax.ppermute only.
A program may use at most 128 MiB of HBM per device.

```python
import math
import jax
import jax.numpy as jnp
import numpy as np
from jax import lax

D = 2048
WIDTH = 1024
BLOCK = 64
NBLK = 16
CONV = 4
FFE = 2048
TOPK = 2
EXPERTS = 16
TOK_A = 32768
MOE_DEV = 128
TOK_B = 32768
CAP = 24


def draw_feature_fading_speeds(key, part):
    first_key, second_key, third_key = jax.random.split(key, 3)
    slow_speed = jnp.exp(jax.random.uniform(first_key, (WIDTH,), jnp.float32, math.log(0.05), math.log(0.2))) / TOK_A
    fast_speed = jnp.exp(jax.random.uniform(second_key, (WIDTH,), jnp.float32, math.log(0.003), math.log(0.01)))
    fast_share = 0.5
    chosen = jax.random.uniform(third_key, (WIDTH,), jnp.float32) < fast_share
    return jnp.where(chosen, fast_speed, slow_speed)


def draw_spike_amount(key, part):
    first_key, second_key = jax.random.split(key)
    places = jax.random.randint(first_key, (8,), 0, TOK_A)
    depth = jnp.log(jax.random.uniform(second_key, (8,), jnp.float32, 0.5, 0.8))
    matches = (jnp.arange(TOK_A, dtype=jnp.int32)[:, None] == places[None, :]).astype(jnp.float32)
    return jnp.sum(matches * depth[None, :], axis=1)


def block_levels(rng, shape, cuts, least, largest):
    def one(dim, parts):
        heights = jax.random.uniform(jax.random.fold_in(jax.random.fold_in(rng, 6), dim), (parts,), jnp.float32, least / len(cuts), largest / len(cuts))
        return jnp.repeat(jnp.exp(heights), shape[dim] // parts).reshape((-1,) + (1,) * (len(shape) - dim - 1))

    gain = one(*cuts[0])
    for cut in cuts[1:]:
        gain = gain * one(*cut)
    return gain


def shared_out(own_key, own, number, rows, count, top, most, skew):
    sequence = jax.random.permutation(own_key, count)
    packed, ordinary = load_shares(count, rows * top, most, skew, True), load_shares(count, rows * top, most, skew, False)
    places = jnp.arange(count)

    def named(tallies, offset_by):
        used = int((tallies > 0).sum())
        fixed = max(1, used // 4)
        shifted = fixed + (places - fixed + offset_by * (used - fixed)) % max(1, count - fixed)
        return jnp.zeros((count,), jnp.int32).at[sequence[jnp.where(places < fixed, places, shifted)]].set(jnp.asarray(tallies, jnp.int32))

    tallies = jnp.where(number % 4 == 0, named(packed, number // 4), named(ordinary, number - number // 4 - 1))
    mixed = jax.random.permutation(jax.random.fold_in(own, 3), count)
    giver, receiver = mixed[0:count // 2 * 2:2], mixed[1:count // 2 * 2:2]
    margin = jnp.minimum(tallies[giver] - 1, most - tallies[receiver]) // 2
    margin = jnp.where((giver == sequence[0]) | (receiver == sequence[0]) | (tallies[receiver] == 0), 0, jnp.maximum(margin, 0))
    shifted = jax.random.randint(jax.random.fold_in(own, 4), (count // 2,), 0, 1 << 20) % (margin + 1)
    tallies = tallies.at[giver].add(-shifted).at[receiver].add(shifted)
    items = jnp.searchsorted(jnp.cumsum(tallies), jnp.arange(rows * top), side="right").astype(jnp.int32)
    table = items.reshape(top, rows).T
    table = table[jax.random.permutation(jax.random.fold_in(own, 1), rows)]
    offset_by = jax.random.randint(jax.random.fold_in(own, 2), (rows, 1), 0, top)
    return jnp.take_along_axis(table, (jnp.arange(top)[None, :] + offset_by) % top, axis=1)


def load_shares(count, total, most, slope, full):
    weights = [(1 << 20) // math.isqrt(grade ** slope) + 1 for grade in range(1, count + 1)]
    largest = most if full else min(most, max(-(-total // count), total * weights[0] // sum(weights)))
    least = 1 if total - largest >= count - 1 else 0
    holding, surplus = [largest] + [least] * (count - 1), total - largest - least * (count - 1)
    while surplus > 0:
        movable = [i for i in range(1, count) if holding[i] < largest] or [i for i in range(1, count) if holding[i] < most]
        whole, remaining = sum([weights[i] for i in movable]), surplus
        for i in movable:
            addition = min(most - holding[i], max(1, remaining * weights[i] // whole), surplus)
            holding[i] = holding[i] + addition
            surplus = surplus - addition
    return np.array(holding)


def noise(stream_key, shape, spread, bound, cuts=(), kind=jnp.bfloat16):
    loudness = block_levels(stream_key, shape, cuts, -0.22, 0.18) if cuts else 1.0
    array = jax.random.normal(stream_key, shape, jnp.float32) * spread * loudness
    return jnp.minimum(jnp.maximum(array, -bound), bound).astype(kind)


def setup_inputs(seed: int = 0) -> dict:
    streams_of = jax.random.split(jax.random.key(seed), 16)
    scan_source_values = noise(streams_of[0], (WIDTH, TOK_A), 1.0, 6.0, ((0, 16), (1, 16)))
    switch_path_values = noise(streams_of[1], (WIDTH, TOK_A), 1.0, 6.0, ((0, 16), (1, 16)))
    causal_filter_coefficients = noise(streams_of[2], (WIDTH, CONV), CONV ** -0.5, 3.0)
    scan_switch_blockmap = noise(streams_of[3], (NBLK, BLOCK, BLOCK), BLOCK ** -0.5, 0.75)
    entry_switch_blockmap = noise(streams_of[4], (NBLK, BLOCK, BLOCK), BLOCK ** -0.5, 0.75)
    feature_fading_speeds = draw_feature_fading_speeds(jax.random.fold_in(streams_of[15], 71), 0)
    spike_amount = draw_spike_amount(jax.random.fold_in(streams_of[15], 71), 0)
    final_linear_map = noise(streams_of[7], (WIDTH, D), WIDTH ** -0.5, 0.1875)
    dispatched_group_activity = noise(streams_of[8], (TOK_B, D), 1.0, 6.0, ((0, 256),))
    specialist_rmsgain = jnp.clip(1.0 + 0.18 * jax.random.normal(streams_of[9], (D,), jnp.float32), 0.099609375, 1.8984375).astype(jnp.bfloat16)
    selected_specialist_ids_keys = jax.random.split(jax.random.fold_in(streams_of[10], 1), TOK_B // MOE_DEV)
    selected_specialist_ids_turns = jax.random.permutation(jax.random.fold_in(streams_of[10], 3), TOK_B // MOE_DEV)
    selected_specialist_ids = jax.vmap(lambda own, number: shared_out(jax.random.fold_in(streams_of[10], 2), own, number, MOE_DEV, EXPERTS, TOPK, CAP, 2))(selected_specialist_ids_keys, selected_specialist_ids_turns).reshape((TOK_B, TOPK))
    selected_specialist_share = jnp.clip(0.2 + 0.8 * jax.random.uniform(streams_of[11], (TOK_B, TOPK), jnp.float32) ** block_levels(streams_of[11], (TOK_B, TOPK), ((0, 256),), -0.2, 0.2), 0.2, 1.0)
    specialist_switch_maps = noise(streams_of[12], (EXPERTS, D, FFE), (D // 6) ** -0.5, 0.3125, ((0, 16), (2, 16)))
    specialist_widen_maps = noise(streams_of[13], (EXPERTS, D, FFE), (D // 6) ** -0.5, 0.3125, ((0, 16), (2, 16)))
    specialist_shrink_maps = noise(streams_of[14], (EXPERTS, D, FFE), (16 * FFE) ** -0.5, 0.03125, ((0, 16), (2, 16)))
    return {"scan_source_values": scan_source_values, "switch_path_values": switch_path_values, "causal_filter_coefficients": causal_filter_coefficients, "scan_switch_blockmap": scan_switch_blockmap, "entry_switch_blockmap": entry_switch_blockmap, "feature_fading_speeds": feature_fading_speeds, "spike_amount": spike_amount, "final_linear_map": final_linear_map, "dispatched_group_activity": dispatched_group_activity, "specialist_rmsgain": specialist_rmsgain, "selected_specialist_ids": selected_specialist_ids, "selected_specialist_share": selected_specialist_share, "specialist_switch_maps": specialist_switch_maps, "specialist_widen_maps": specialist_widen_maps, "specialist_shrink_maps": specialist_shrink_maps}


def combine_pairs(earlier, later):
    return (earlier[0] * later[0], later[0] * earlier[1] + later[1])

def scan_path(scan_source_values, switch_path_values, causal_filter_coefficients, scan_switch_blockmap, entry_switch_blockmap, feature_fading_speeds, spike_amount, final_linear_map):
    positions = scan_source_values.shape[1]
    padded = jnp.pad(scan_source_values.astype(jnp.float32), ((0, 0), (CONV - 1, 0)))
    conv_taps = causal_filter_coefficients.astype(jnp.float32)
    running = padded[:, 0:positions] * conv_taps[:, 0:1]
    for shift_tap in range(1, CONV):
        running = running + padded[:, shift_tap:shift_tap + positions] * conv_taps[:, shift_tap:shift_tap + 1]
    conv_out = running.astype(jnp.bfloat16)
    grouped = conv_out.astype(jnp.float32).reshape(NBLK, BLOCK, positions)
    scan_switch = jax.nn.sigmoid(jnp.einsum('gij,git->gjt', scan_switch_blockmap.astype(jnp.float32), grouped).reshape(WIDTH, positions))
    inflow = jax.nn.sigmoid(jnp.einsum('gij,git->gjt', entry_switch_blockmap.astype(jnp.float32), grouped).reshape(WIDTH, positions))
    fading_exponent = -8.0 * scan_switch * feature_fading_speeds[:, None] + spike_amount[None, :]
    drive = jnp.sqrt(-jnp.expm1(2.0 * fading_exponent)) * inflow * conv_out.astype(jnp.float32)
    unused, state = lax.associative_scan(combine_pairs, (jnp.exp(fading_exponent), drive), axis=1)
    mix_hidden = (state * jax.nn.gelu(switch_path_values.astype(jnp.float32), approximate=True)).astype(jnp.bfloat16)
    return jnp.dot(mix_hidden.T, final_linear_map, preferred_element_type=jnp.float32).astype(jnp.bfloat16)

def expert_branch(dispatched_group_activity, specialist_rmsgain, selected_specialist_ids, selected_specialist_share, specialist_switch_maps, specialist_widen_maps, specialist_shrink_maps):
    values = dispatched_group_activity.astype(jnp.float32)
    scale = lax.rsqrt(lax.optimization_barrier(jnp.mean(values * values, axis=1, keepdims=True)) + 1e-06)
    normed = (values * scale * specialist_rmsgain.astype(jnp.float32)).astype(jnp.bfloat16)
    token_total, route_count = selected_specialist_ids.shape
    model_width = dispatched_group_activity.shape[1]
    block_count = token_total // MOE_DEV
    flat_ids = selected_specialist_ids.reshape(block_count, MOE_DEV * route_count)
    one_hot = (flat_ids[:, :, None] == jnp.arange(EXPERTS, dtype=jnp.int32)[None, None, :]).astype(jnp.int32)
    slot_rank = lax.optimization_barrier(jnp.sum((jnp.cumsum(one_hot, axis=1) - one_hot) * one_hot, axis=2))
    owner_token = jnp.arange(block_count, dtype=jnp.int32)[:, None] * MOE_DEV + jnp.arange(MOE_DEV * route_count, dtype=jnp.int32)[None, :] // route_count
    flat_weight = selected_specialist_share.reshape(block_count, MOE_DEV * route_count)
    padded_rows = jnp.concatenate([normed, jnp.zeros((1, model_width), jnp.bfloat16)], axis=0)
    slot_total = block_count * CAP

    def one_expert(running, expert):
        mine = flat_ids == expert
        slot_index = jnp.where(mine, jnp.arange(block_count, dtype=jnp.int32)[:, None] * CAP + slot_rank, slot_total).astype(jnp.int32)
        slot_token = jnp.full((slot_total + 1,), token_total, jnp.int32).at[slot_index.reshape(-1)].set(owner_token.reshape(-1))[:slot_total]
        slot_weight = jnp.zeros((slot_total + 1,), jnp.float32).at[slot_index.reshape(-1)].set(flat_weight.reshape(-1))[:slot_total]
        rows = padded_rows[jnp.minimum(slot_token, token_total)]
        gate_pre = jnp.dot(rows, specialist_switch_maps[expert], preferred_element_type=jnp.float32)
        up_pre = jnp.dot(rows, specialist_widen_maps[expert], preferred_element_type=jnp.float32)
        gate_cut = jnp.minimum(gate_pre, 7.0)
        up_cut = jnp.clip(up_pre, -7.0, 7.0)
        units = ((up_cut + 1.0) * gate_cut * jax.nn.sigmoid(1.702 * gate_cut)).astype(jnp.bfloat16)
        result = lax.dot_general(units, specialist_shrink_maps[expert], (((1,), (1,)), ((), ())), preferred_element_type=jnp.float32).astype(jnp.bfloat16)
        running = running.at[slot_token].add(result.astype(jnp.float32) * slot_weight[:, None], mode='drop')
        return (running, None)
    running, unused = lax.scan(one_expert, jnp.zeros((token_total, model_width), jnp.float32), jnp.arange(EXPERTS, dtype=jnp.int32))
    return running.astype(jnp.bfloat16)

def reference(scan_source_values, switch_path_values, causal_filter_coefficients, scan_switch_blockmap, entry_switch_blockmap, feature_fading_speeds, spike_amount, final_linear_map, dispatched_group_activity, specialist_rmsgain, selected_specialist_ids, selected_specialist_share, specialist_switch_maps, specialist_widen_maps, specialist_shrink_maps):
    scan_path_result = scan_path(scan_source_values, switch_path_values, causal_filter_coefficients, scan_switch_blockmap, entry_switch_blockmap, feature_fading_speeds, spike_amount, final_linear_map)
    moe_out = expert_branch(dispatched_group_activity, specialist_rmsgain, selected_specialist_ids, selected_specialist_share, specialist_switch_maps, specialist_widen_maps, specialist_shrink_maps)
    return (scan_path_result, moe_out)
```

```python
import jax
import jax.numpy as jnp
from jax import lax
from jax.experimental import pallas as pl
from jax.experimental.pallas import tpu as pltpu
from jax.sharding import PartitionSpec as P


LANES = 128
TILES_AT_ONCE = 4
CUT = 512


def from_everyone(x, axis):
    copies = jnp.broadcast_to(x, (lax.axis_size(axis), *x.shape))
    return lax.all_to_all(copies, axis, split_axis=0, concat_axis=0, tiled=True)


def from_behind(x, axis, by):
    count = lax.axis_size(axis)
    pairs = [(i, i + by) for i in range(count) if 0 <= i + by < count]
    return lax.ppermute(x, axis, pairs)


def along_z(x, by):
    tp = lax.axis_size("tp")
    return lax.ppermute(x, "tp", [(i, (i + 2 * by) % tp) for i in range(tp)])


def other_core(x):
    tp = lax.axis_size("tp")
    return lax.ppermute(x, "tp", [(i, i ^ 1) for i in range(tp)])


def times(a, b):
    return jnp.dot(a, b, preferred_element_type=jnp.float32)


def times_t(a, b):
    return lax.dot_general(a, b, (((1,), (1,)), ((), ())), preferred_element_type=jnp.float32)


def cost(flops, moved):
    return pl.CostEstimate(flops=flops, bytes_accessed=moved, transcendentals=0)


def minus_expm1(v, exp_v):
    series = 1.0 + v * (1.0 / 9.0)
    for k in range(8, 1, -1):
        series = 1.0 + v * (1.0 / k) * series
    return jnp.where(v > -0.5, -v * series, 1.0 - exp_v)


def local_scan(x, halo, taps, rate_map, entry_map, fade, spike, group):
    channels, positions = x.shape
    block = rate_map.shape[1]

    def body(_, x_ref, halo_ref, taps_ref, rate_ref, entry_ref, fade_ref, spike_ref, decay_ref, state_ref, total_ref, map_ref):
        map_ref[:block] = rate_ref[0].astype(jnp.float32).T.astype(jnp.bfloat16)
        map_ref[block:] = entry_ref[0].astype(jnp.float32).T.astype(jnp.bfloat16)
        lane = lax.broadcasted_iota(jnp.int32, (channels, LANES), 1)
        tap = [taps_ref[:, k : k + 1].astype(jnp.float32) for k in range(4)]
        speed = -8.0 * fade_ref[...]

        def rolled(a):
            return [pltpu.roll(a, s, 1) for s in (1, 2, 3)]

        def steps(chunk, carry):
            decay_run, state_run, before = carry[0], carry[1], list(carry[2:])
            found = []
            for t in range(TILES_AT_ONCE):
                at = pl.ds(pl.multiple_of((chunk * TILES_AT_ONCE + t) * LANES, LANES), LANES)
                here = x_ref[:, at].astype(jnp.float32)
                moved = rolled(here)
                conv = here * tap[3]
                for s in (1, 2, 3):
                    conv = conv + tap[3 - s] * jnp.where(lane < s, before[s - 1], moved[s - 1])
                before = moved
                conv = conv.astype(jnp.bfloat16)
                gates = times(map_ref[...], conv)
                rate = jax.nn.sigmoid(gates[:block])
                inflow = jax.nn.sigmoid(gates[block:])
                exponent = rate * speed + spike_ref[:, at]
                decay = jnp.exp(exponent)
                share = minus_expm1(2.0 * exponent, decay * decay)
                root = jnp.where(share > 0.0, jnp.sqrt(share), 0.0)
                state = root * inflow * conv.astype(jnp.float32)
                k = 1
                while k < LANES:
                    inside = lane >= k
                    state = state + jnp.where(inside, decay * pltpu.roll(state, k, 1), 0.0)
                    decay = decay * jnp.where(inside, pltpu.roll(decay, k, 1), 1.0)
                    k *= 2
                found.append((at, decay, state))
            for at, decay, state in found:
                state = state + decay * state_run
                decay = decay * decay_run
                decay_ref[:, at] = decay
                state_ref[:, at] = state
                decay_run = jnp.broadcast_to(decay[:, LANES - 1 :], decay.shape)
                state_run = jnp.broadcast_to(state[:, LANES - 1 :], state.shape)
            return (decay_run, state_run, *before)

        one = jnp.ones((channels, LANES), jnp.float32)
        first = (one, jnp.zeros_like(one), *rolled(halo_ref[...].astype(jnp.float32)))
        last = lax.fori_loop(0, positions // (LANES * TILES_AT_ONCE), steps, first)
        ends = jnp.where(lane == 0, last[0], jnp.where(lane == 1, last[1], 0.0))
        total_ref[...] = ends.T[:8]

    whole = lambda *shape: pl.BlockSpec(shape, lambda i, g: (0,) * len(shape))
    return pl.pallas_call(
        body,
        grid_spec=pltpu.PrefetchScalarGridSpec(
            num_scalar_prefetch=1,
            grid=(1,),
            in_specs=[
                whole(channels, positions),
                whole(channels, LANES),
                pl.BlockSpec((channels, 4), lambda i, g: (g[0], 0)),
                pl.BlockSpec((1, block, block), lambda i, g: (g[0], 0, 0)),
                pl.BlockSpec((1, block, block), lambda i, g: (g[0], 0, 0)),
                pl.BlockSpec((channels, 1), lambda i, g: (g[0], 0)),
                whole(1, positions),
            ],
            out_specs=[
                whole(channels, positions),
                whole(channels, positions),
                whole(8, channels),
            ],
            scratch_shapes=[pltpu.VMEM((2 * block, block), jnp.bfloat16)],
        ),
        out_shape=[
            jax.ShapeDtypeStruct((channels, positions), jnp.float32),
            jax.ShapeDtypeStruct((channels, positions), jnp.float32),
            jax.ShapeDtypeStruct((8, channels), jnp.float32),
        ],
        cost_estimate=cost(4 * 10**9, 2 * 10**6),
        compiler_params=pltpu.CompilerParams(vmem_limit_bytes=12 * 2**20),
        name="local_scan",
    )(group, x, halo, taps, rate_map, entry_map, fade, spike)


def gated_states(decay, state, switch, totals, place, pieces):
    channels, positions = decay.shape
    width = positions // pieces

    def body(place_ref, decay_ref, state_ref, switch_ref, totals_ref, out_ref):
        entering = jnp.zeros((1, channels), jnp.float32)
        for b in range(totals.shape[0]):
            passed = b < place_ref[0]
            entering = jnp.where(
                passed, totals_ref[b, 0:1] * entering + totals_ref[b, 1:2], entering
            )
        entering = jnp.broadcast_to(entering, (LANES, channels)).T
        for p in range(pieces):
            at = slice(p * width, (p + 1) * width)
            whole = state_ref[:, at] + decay_ref[:, at] * entering
            gate = jax.nn.gelu(switch_ref[:, at].astype(jnp.float32), approximate=True)
            out_ref[p] = (whole * gate).astype(jnp.bfloat16)

    vmem = pl.BlockSpec(memory_space=pltpu.VMEM)
    return pl.pallas_call(
        body,
        in_specs=[pl.BlockSpec(memory_space=pltpu.SMEM)] + [vmem] * 4,
        out_specs=vmem,
        out_shape=jax.ShapeDtypeStruct((pieces, channels, width), jnp.bfloat16),
        cost_estimate=cost(10**9, 2 * 10**6),
        compiler_params=pltpu.CompilerParams(vmem_limit_bytes=12 * 2**20),
        name="gated_states",
    )(place, decay, state, switch, totals)


def mixer_half(
    scan_source_values,
    switch_path_values,
    causal_filter_coefficients,
    scan_switch_blockmap,
    entry_switch_blockmap,
    feature_fading_speeds,
    spike_amount,
    final_linear_map,
):
    halo = from_behind(scan_source_values[:, -LANES:], "ep", 1)
    decay, state, total = local_scan(
        scan_source_values,
        halo,
        causal_filter_coefficients,
        scan_switch_blockmap,
        entry_switch_blockmap,
        feature_fading_speeds[:, None],
        spike_amount[None, :],
        lax.axis_index("tp").astype(jnp.int32)[None],
    )
    pieces = gated_states(
        decay,
        state,
        switch_path_values,
        from_everyone(total, "ep"),
        lax.axis_index("ep").astype(jnp.int32)[None],
        lax.axis_size("tp"),
    )
    mixed = lax.all_to_all(pieces, "tp", split_axis=0, concat_axis=0, tiled=True)
    return lax.dot_general(
        mixed.reshape(-1, mixed.shape[2]),
        final_linear_map,
        (((0,), (0,)), ((), ())),
        preferred_element_type=jnp.float32,
    ).astype(jnp.bfloat16)


def token_rows(activity, gain, ids, share, experts, slots):
    tokens, width = activity.shape

    def body(act_ref, gain_ref, ids_ref, share_ref, rows_ref, back_ref):
        values = act_ref[...].astype(jnp.float32)
        scale = lax.rsqrt(jnp.mean(values * values, axis=1, keepdims=True) + 1e-06)
        normed = (values * scale * gain_ref[...].astype(jnp.float32)).astype(jnp.bfloat16)
        expert = lax.broadcasted_iota(jnp.int32, (experts, tokens), 0)
        earlier = lax.broadcasted_iota(jnp.int32, (tokens, tokens), 0)
        later = lax.broadcasted_iota(jnp.int32, (tokens, tokens), 1)
        ahead = (earlier < later).astype(jnp.float32).astype(jnp.bfloat16)
        slot = lax.broadcasted_iota(jnp.int32, (experts * slots, tokens), 0)
        count = jnp.zeros((experts, 1), jnp.float32)
        taken = jnp.zeros((experts * slots, tokens), jnp.float32)
        back = jnp.zeros((experts * slots, tokens), jnp.float32)
        for j in range(ids.shape[0]):
            mine = (expert == ids_ref[j : j + 1]).astype(jnp.float32)
            rank = times(mine.astype(jnp.bfloat16), ahead) + count
            rank = jnp.sum(mine * rank, axis=0, keepdims=True)
            count = count + jnp.sum(mine, axis=1, keepdims=True)
            here = slot == ids_ref[j : j + 1] * slots + rank.astype(jnp.int32)
            taken = taken + jnp.where(here, 1.0, 0.0)
            back = back + jnp.where(here, share_ref[j : j + 1], 0.0)
        rows_ref[...] = times(taken.astype(jnp.bfloat16), normed).astype(jnp.bfloat16)
        rest = back.T
        for k in range(3):
            part = rest.astype(jnp.bfloat16)
            back_ref[k] = part
            rest = rest - part.astype(jnp.float32)

    return pl.pallas_call(
        body,
        out_shape=[
            jax.ShapeDtypeStruct((experts * slots, width), jnp.bfloat16),
            jax.ShapeDtypeStruct((3, tokens, experts * slots), jnp.bfloat16),
        ],
        cost_estimate=cost(10**9, 2 * 10**6),
        compiler_params=pltpu.CompilerParams(vmem_limit_bytes=12 * 2**20),
        name="token_rows",
    )(activity, gain, ids, share)


def weighted_sum(back, results):
    parts, tokens, slots = back.shape
    width = results.shape[1]

    def body(back_ref, results_ref, out_ref):
        total = times(back_ref[0], results_ref[...])
        for k in range(1, parts):
            total = total + times(back_ref[k], results_ref[...])
        out_ref[...] = total.astype(jnp.bfloat16)

    return pl.pallas_call(
        body,
        out_shape=jax.ShapeDtypeStruct((tokens, width), jnp.bfloat16),
        cost_estimate=cost(2 * parts * tokens * slots * width, 2 * slots * width),
        compiler_params=pltpu.CompilerParams(vmem_limit_bytes=12 * 2**20),
        name="weighted_sum",
    )(back, results)


def near(x):
    return pltpu.with_memory_space_constraint(x, pltpu.VMEM)


def gated(gate_pre, up_pre):
    gate_cut = jnp.minimum(gate_pre, 7.0)
    up_cut = jnp.clip(up_pre, -7.0, 7.0)
    return ((up_cut + 1.0) * gate_cut * jax.nn.sigmoid(1.702 * gate_cut)).astype(jnp.bfloat16)


def expert_step(rows, shards, so_far, dtype):
    sets, count, width = len(rows), *rows[0].shape
    placed = pltpu.VMEM if dtype == jnp.float32 else jax.ShapeDtypeStruct
    hidden = shards[0][0][0].shape[1]
    operands, layout = [], []
    for shard in shards:
        layout.append([])
        for pieces in shard:
            layout[-1].append((len(operands), len(pieces)))
            operands += pieces

    def body(*refs):
        row_refs, weights = refs[:sets], refs[sets : sets + len(operands)]
        refs = refs[sets + len(operands) :]
        old, new = (refs[:sets], refs[sets:]) if so_far else ((), refs)

        def load(at):
            return jnp.concatenate([weights[at[0] + k][...] for k in range(at[1])], axis=0)

        def side_by_side(ats):
            return jnp.concatenate([load(at) for at in ats], axis=1)

        for k in range(sets):
            first = 0
            while first < len(shards):
                taken = layout[first : first + 2]
                base = old if first == 0 else new
                if len(taken) == 2:
                    gate_pre = times(row_refs[k][...], side_by_side([s[0] for s in taken]))
                    up_pre = times(row_refs[k][...], side_by_side([s[1] for s in taken]))
                else:
                    both = times(row_refs[k][...], side_by_side(taken[0][:2]))
                    gate_pre, up_pre = both[:, :hidden], both[:, hidden:]
                units = gated(gate_pre, up_pre)
                down = side_by_side([s[2] for s in taken])
                for at in range(0, width, CUT):
                    added = times_t(units, down[at : at + CUT])
                    if base:
                        added = base[k][:, at : at + CUT] + added
                    new[k][:, at : at + CUT] = added.astype(dtype)
                first += 2

    alias = {sets + len(operands) + k: k for k in range(sets)} if so_far and dtype == jnp.float32 else {}
    return pl.pallas_call(
        body,
        in_specs=[pl.BlockSpec(memory_space=pltpu.VMEM)] * (sets + len(operands) + len(so_far)),
        out_specs=[pl.BlockSpec(memory_space=pltpu.VMEM)] * sets,
        out_shape=[placed((count, width), dtype)] * sets,
        input_output_aliases=alias,
        cost_estimate=cost(
            2 * sets * count * 3 * width * hidden * len(shards), 6 * width * hidden * len(shards)
        ),
        compiler_params=pltpu.CompilerParams(vmem_limit_bytes=24 * 2**20),
    )(*map(near, rows), *operands, *map(near, so_far))


def z_ring(own):
    chips = lax.axis_size("tp") // 2
    up, down, found = own, own, []

    def moved(arrays, by):
        return [along_z(a, by) for a in arrays]

    for _ in range(1, chips // 2):
        up, down = moved(up, 1), moved(down, -1)
        found.append([[(a,) for a in up], [(a,) for a in down]])
    half = own[0].shape[0] // 2
    up = moved([a[:half] for a in up], 1)
    down = moved([a[half:] for a in down], -1)
    return found, list(zip(up, down))


def expert_half(
    dispatched_group_activity,
    specialist_rmsgain,
    selected_specialist_ids,
    selected_specialist_share,
    specialist_switch_maps,
    specialist_widen_maps,
    specialist_shrink_maps,
):
    token_count, model_width = dispatched_group_activity.shape
    route_count = selected_specialist_ids.shape[1]
    expert_count = lax.axis_size("ep")
    slot_count = 3 * route_count * token_count // (2 * expert_count)
    own = [specialist_switch_maps[0], specialist_widen_maps[0], specialist_shrink_maps[0]]
    found, opposite = z_ring(own)
    outgoing, back = token_rows(
        dispatched_group_activity,
        specialist_rmsgain[None, :],
        selected_specialist_ids.T,
        selected_specialist_share.T,
        expert_count,
        slot_count,
    )

    def exchange(rows):
        blocks = rows.reshape(expert_count, slot_count, model_width)
        return lax.all_to_all(blocks, "ep", split_axis=0, concat_axis=0, tiled=True).reshape(
            expert_count * slot_count, model_width
        )

    kept = exchange(outgoing)
    lent = other_core(kept)
    found[0].append([(a,) for a in own])
    partial = ()
    for shards in found:
        partial = expert_step((lent, kept), shards, tuple(partial), jnp.float32)
    (sent,) = expert_step((lent,), [opposite], partial[:1], jnp.bfloat16)
    back_home = other_core(sent)
    (mine,) = expert_step((kept,), [opposite], partial[1:], jnp.float32)
    result = (mine + back_home.astype(jnp.float32)).astype(jnp.bfloat16)
    return weighted_sum(back, exchange(result))


def on_device(
    scan_source_values,
    switch_path_values,
    causal_filter_coefficients,
    scan_switch_blockmap,
    entry_switch_blockmap,
    feature_fading_speeds,
    spike_amount,
    final_linear_map,
    dispatched_group_activity,
    specialist_rmsgain,
    selected_specialist_ids,
    selected_specialist_share,
    specialist_switch_maps,
    specialist_widen_maps,
    specialist_shrink_maps,
):
    scan_path_result = mixer_half(
        scan_source_values,
        switch_path_values,
        causal_filter_coefficients,
        scan_switch_blockmap,
        entry_switch_blockmap,
        feature_fading_speeds,
        spike_amount,
        final_linear_map,
    )
    moe_out = expert_half(
        dispatched_group_activity,
        specialist_rmsgain,
        selected_specialist_ids,
        selected_specialist_share,
        specialist_switch_maps,
        specialist_widen_maps,
        specialist_shrink_maps,
    )
    return (scan_path_result, moe_out)


def solution(mesh):
    in_specs = (
        P("tp", "ep"),
        P("tp", "ep"),
        P(),
        P(),
        P(),
        P(),
        P("ep"),
        P(),
        P(("ep", "tp"), None),
        P(),
        P(("ep", "tp"), None),
        P(("ep", "tp"), None),
        P("ep", None, "tp"),
        P("ep", None, "tp"),
        P("ep", None, "tp"),
    )
    out_specs = (P(("ep", "tp"), None), P(("ep", "tp"), None))
    return jax.shard_map(
        lambda *args: on_device(*args), mesh=mesh, in_specs=in_specs, out_specs=out_specs, check_vma=False
    )
```

```python
import jax
import jax.numpy as jnp
from jax import lax
from jax.experimental import pallas as pl
from jax.experimental.pallas import tpu as pltpu
from jax.sharding import PartitionSpec as P


LANES = 128
TILES_AT_ONCE = 4
CUT = 512
STEP_MIB = 12


def swapped(x, axis):
    return lax.all_to_all(x, axis, split_axis=0, concat_axis=0, tiled=True)


def from_behind(x, axis, by):
    count = lax.axis_size(axis)
    pairs = [(i, i + by) for i in range(count) if 0 <= i + by < count]
    return lax.ppermute(x, axis, pairs)


def along_z(x, by):
    tp = lax.axis_size("tp")
    return lax.ppermute(x, "tp", [(i, (i + (2 * by if i % 2 == 0 else -2 * by)) % tp) for i in range(tp)])


def other_core(x):
    tp = lax.axis_size("tp")
    return lax.ppermute(x, "tp", [(i, i ^ 1) for i in range(tp)])


def times(a, b):
    return jnp.dot(a, b, preferred_element_type=jnp.float32)


def times_t(a, b):
    return lax.dot_general(a, b, (((1,), (1,)), ((), ())), preferred_element_type=jnp.float32)


def far(x):
    return pltpu.with_memory_space_constraint(x, pltpu.HBM)


def cost(flops, moved):
    return pl.CostEstimate(flops=flops, bytes_accessed=moved, transcendentals=0)


def minus_expm1(v, exp_v):
    series = 1.0 + v * (1.0 / 9.0)
    for k in range(8, 1, -1):
        series = 1.0 + v * (1.0 / k) * series
    return jnp.where(v > -0.5, -v * series, 1.0 - exp_v)


def local_scan(x, halo, taps, rate_map, entry_map, fade, spike, group, blocks):
    channels, positions = x.shape
    block = rate_map.shape[1]

    def body(group_ref, x_ref, halo_ref, taps_ref, rate_ref, entry_ref, fade_ref, spike_ref, decay_ref, state_ref, total_ref, map_ref):
        map_ref[:block] = rate_ref[0].astype(jnp.float32).T.astype(jnp.bfloat16)
        map_ref[block:] = entry_ref[0].astype(jnp.float32).T.astype(jnp.bfloat16)
        lane = lax.broadcasted_iota(jnp.int32, (channels, LANES), 1)
        group = group_ref[0]
        per_row = LANES // channels

        def column(row):
            row = jnp.where(group % per_row == 0, row, pltpu.roll(row, LANES - channels, 1))
            return jnp.broadcast_to(row, (LANES, LANES)).T[:channels]

        at = pl.ds(pl.multiple_of(group // per_row * LANES, LANES), LANES)
        here = taps_ref[:, at].astype(jnp.float32)
        tap = [column(here[k : k + 1]) for k in range(4)]
        speed = -8.0 * column(fade_ref[pl.ds(group // per_row, 1), :])

        def rolled(a):
            return [pltpu.roll(a, s, 1) for s in (1, 2, 3)]

        def steps(chunk, carry):
            decay_run, state_run, before = carry[0], carry[1], list(carry[2:])
            found = []
            for t in range(TILES_AT_ONCE):
                at = pl.ds(pl.multiple_of((chunk * TILES_AT_ONCE + t) * LANES, LANES), LANES)
                here = x_ref[:, at].astype(jnp.float32)
                moved = rolled(here)
                conv = here * tap[3]
                for s in (1, 2, 3):
                    conv = conv + tap[3 - s] * jnp.where(lane < s, before[s - 1], moved[s - 1])
                before = moved
                conv = conv.astype(jnp.bfloat16)
                gates = times(map_ref[...], conv)
                rate = jax.nn.sigmoid(gates[:block])
                inflow = jax.nn.sigmoid(gates[block:])
                exponent = rate * speed + spike_ref[:, at]
                decay = jnp.exp(exponent)
                share = minus_expm1(2.0 * exponent, decay * decay)
                root = jnp.where(share > 0.0, jnp.sqrt(share), 0.0)
                state = root * inflow * conv.astype(jnp.float32)
                k = 1
                while k < LANES:
                    inside = lane >= k
                    state = state + jnp.where(inside, decay * pltpu.roll(state, k, 1), 0.0)
                    decay = decay * jnp.where(inside, pltpu.roll(decay, k, 1), 1.0)
                    k *= 2
                found.append((at, decay, state))
            for at, decay, state in found:
                state = state + decay * state_run
                decay = decay * decay_run
                decay_ref[:, at] = decay
                state_ref[:, at] = state
                decay_run = jnp.broadcast_to(decay[:, LANES - 1 :], decay.shape)
                state_run = jnp.broadcast_to(state[:, LANES - 1 :], state.shape)
            return (decay_run, state_run, *before)

        one = jnp.ones((channels, LANES), jnp.float32)
        first = (one, jnp.zeros_like(one), *rolled(halo_ref[...].astype(jnp.float32)))
        last = lax.fori_loop(0, positions // (LANES * TILES_AT_ONCE), steps, first)
        ends = jnp.where(lane == 0, last[0], jnp.where(lane == 1, last[1], 0.0))
        ends = jnp.concatenate([ends, jnp.zeros_like(ends)], axis=0).T[:8]
        total_ref[...] = jnp.broadcast_to(ends, total_ref.shape)

    whole = lambda *shape: pl.BlockSpec(shape, lambda i, g: (0,) * len(shape))
    return pl.pallas_call(
        body,
        grid_spec=pltpu.PrefetchScalarGridSpec(
            num_scalar_prefetch=1,
            grid=(1,),
            in_specs=[
                whole(channels, positions),
                whole(channels, LANES),
                whole(*taps.shape),
                pl.BlockSpec((1, block, block), lambda i, g: (g[0], 0, 0)),
                pl.BlockSpec((1, block, block), lambda i, g: (g[0], 0, 0)),
                whole(*fade.shape),
                whole(1, positions),
            ],
            out_specs=[
                whole(channels, positions),
                whole(channels, positions),
                whole(blocks, 8, LANES),
            ],
            scratch_shapes=[pltpu.VMEM((2 * block, block), jnp.bfloat16)],
        ),
        out_shape=[
            jax.ShapeDtypeStruct((channels, positions), jnp.float32),
            jax.ShapeDtypeStruct((channels, positions), jnp.float32),
            jax.ShapeDtypeStruct((blocks, 8, LANES), jnp.float32),
        ],
        cost_estimate=cost(4 * 10**9, 2 * 10**6),
        compiler_params=pltpu.CompilerParams(vmem_limit_bytes=12 * 2**20),
        name="local_scan",
    )(group, far(x), halo, far(taps), far(rate_map), far(entry_map), far(fade), far(spike))


def gated_states(decay, state, switch, totals, place, pieces):
    channels, positions = decay.shape
    width = positions // pieces

    def body(place_ref, decay_ref, state_ref, switch_ref, totals_ref, out_ref):
        entering = jnp.zeros((1, LANES), jnp.float32)
        for b in range(totals.shape[0]):
            passed = b < place_ref[0]
            entering = jnp.where(
                passed, totals_ref[b, 0:1] * entering + totals_ref[b, 1:2], entering
            )
        entering = jnp.broadcast_to(entering, (LANES, LANES)).T[:channels]
        for p in range(pieces):
            at = slice(p * width, (p + 1) * width)
            whole = state_ref[:, at] + decay_ref[:, at] * entering
            gate = jax.nn.gelu(switch_ref[:, at].astype(jnp.float32), approximate=True)
            out_ref[p] = (whole * gate).astype(jnp.bfloat16)

    vmem = pl.BlockSpec(memory_space=pltpu.VMEM)
    return pl.pallas_call(
        body,
        in_specs=[pl.BlockSpec(memory_space=pltpu.SMEM)] + [vmem] * 4,
        out_specs=vmem,
        out_shape=jax.ShapeDtypeStruct((pieces, channels, width), jnp.bfloat16),
        cost_estimate=cost(10**9, 2 * 10**6),
        compiler_params=pltpu.CompilerParams(vmem_limit_bytes=12 * 2**20),
        name="gated_states",
    )(place, decay, state, far(switch), totals)


def mixer_half(
    scan_source_values,
    switch_path_values,
    causal_filter_coefficients,
    scan_switch_blockmap,
    entry_switch_blockmap,
    feature_fading_speeds,
    spike_amount,
    final_linear_map,
):
    halo = from_behind(scan_source_values[:, -LANES:], "ep", 1)
    decay, state, total = local_scan(
        scan_source_values,
        halo,
        causal_filter_coefficients.T,
        scan_switch_blockmap,
        entry_switch_blockmap,
        feature_fading_speeds.reshape(-1, LANES),
        spike_amount[None, :],
        lax.axis_index("tp").astype(jnp.int32)[None],
        lax.axis_size("ep"),
    )
    pieces = gated_states(
        decay,
        state,
        switch_path_values,
        swapped(total, "ep"),
        lax.axis_index("ep").astype(jnp.int32)[None],
        lax.axis_size("tp"),
    )
    mixed = lax.all_to_all(pieces, "tp", split_axis=0, concat_axis=0, tiled=True)
    return lax.dot_general(
        mixed.reshape(-1, mixed.shape[2]),
        final_linear_map,
        (((0,), (0,)), ((), ())),
        preferred_element_type=jnp.float32,
    ).astype(jnp.bfloat16)


def token_rows(activity, gain, ids, share, experts, slots):
    tokens, width = activity.shape

    def body(act_ref, gain_ref, ids_ref, share_ref, rows_ref, back_ref):
        values = act_ref[...].astype(jnp.float32)
        scale = lax.rsqrt(jnp.mean(values * values, axis=1, keepdims=True) + 1e-06)
        normed = (values * scale * gain_ref[...].astype(jnp.float32)).astype(jnp.bfloat16)
        expert = lax.broadcasted_iota(jnp.int32, (experts, tokens), 0)
        earlier = lax.broadcasted_iota(jnp.int32, (tokens, tokens), 0)
        later = lax.broadcasted_iota(jnp.int32, (tokens, tokens), 1)
        ahead = (earlier < later).astype(jnp.float32).astype(jnp.bfloat16)
        slot = lax.broadcasted_iota(jnp.int32, (experts * slots, tokens), 0)
        count = jnp.zeros((experts, 1), jnp.float32)
        taken = jnp.zeros((experts * slots, tokens), jnp.float32)
        back = jnp.zeros((experts * slots, tokens), jnp.float32)
        for j in range(ids.shape[0]):
            mine = (expert == ids_ref[j : j + 1]).astype(jnp.float32)
            rank = times(mine.astype(jnp.bfloat16), ahead) + count
            rank = jnp.sum(mine * rank, axis=0, keepdims=True)
            count = count + jnp.sum(mine, axis=1, keepdims=True)
            here = slot == ids_ref[j : j + 1] * slots + rank.astype(jnp.int32)
            taken = taken + jnp.where(here, 1.0, 0.0)
            back = back + jnp.where(here, share_ref[j : j + 1], 0.0)
        rows_ref[...] = times(taken.astype(jnp.bfloat16), normed).astype(jnp.bfloat16)
        rest = back.T
        for k in range(3):
            part = rest.astype(jnp.bfloat16)
            back_ref[k] = part
            rest = rest - part.astype(jnp.float32)

    return pl.pallas_call(
        body,
        out_shape=[
            jax.ShapeDtypeStruct((experts * slots, width), jnp.bfloat16),
            jax.ShapeDtypeStruct((3, tokens, experts * slots), jnp.bfloat16),
        ],
        cost_estimate=cost(10**9, 2 * 10**6),
        compiler_params=pltpu.CompilerParams(vmem_limit_bytes=12 * 2**20),
        name="token_rows",
    )(far(activity), gain, far(ids), far(share))


def weighted_sum(back, results):
    parts, tokens, slots = back.shape
    width = results.shape[1]

    def body(back_ref, results_ref, out_ref):
        total = times(back_ref[0], results_ref[...])
        for k in range(1, parts):
            total = total + times(back_ref[k], results_ref[...])
        out_ref[...] = total.astype(jnp.bfloat16)

    return pl.pallas_call(
        body,
        out_shape=jax.ShapeDtypeStruct((tokens, width), jnp.bfloat16),
        cost_estimate=cost(2 * parts * tokens * slots * width, 2 * slots * width),
        compiler_params=pltpu.CompilerParams(vmem_limit_bytes=12 * 2**20),
        name="weighted_sum",
    )(back, results)


def near(x):
    return pltpu.with_memory_space_constraint(x, pltpu.VMEM)


def gated(gate_pre, up_pre):
    gate_cut = jnp.minimum(gate_pre, 7.0)
    up_cut = jnp.clip(up_pre, -7.0, 7.0)
    return ((up_cut + 1.0) * gate_cut * jax.nn.sigmoid(1.702 * gate_cut)).astype(jnp.bfloat16)


def expert_step(rows, shards, so_far):
    sets, count, width = len(rows), *rows[0].shape
    hidden = shards[0][0].shape[1]
    operands = [a for shard in shards for a in shard]
    layout = [(3 * k, 3 * k + 1, 3 * k + 2) for k in range(len(shards))]

    def body(*refs):
        row_refs, weights = refs[:sets], refs[sets : sets + len(operands)]
        refs = refs[sets + len(operands) :]
        old, new = (refs[:sets], refs[sets:]) if so_far else ((), refs)

        def side_by_side(ats):
            return jnp.concatenate([weights[at][...] for at in ats], axis=1)

        for k in range(sets):
            first = 0
            while first < len(shards):
                taken = layout[first : first + 2]
                base = old if first == 0 else new
                if len(taken) == 2:
                    gate_pre = times(row_refs[k][...], side_by_side([s[0] for s in taken]))
                    up_pre = times(row_refs[k][...], side_by_side([s[1] for s in taken]))
                else:
                    both = times(row_refs[k][...], side_by_side(taken[0][:2]))
                    gate_pre, up_pre = both[:, :hidden], both[:, hidden:]
                units = gated(gate_pre, up_pre)
                down = side_by_side([s[2] for s in taken])
                for at in range(0, width, CUT):
                    added = times_t(units, down[at : at + CUT])
                    if base:
                        added = base[k][:, at : at + CUT] + added
                    new[k][:, at : at + CUT] = added
                first += 2

    alias = {sets + len(operands) + k: k for k in range(sets)} if so_far else {}
    return pl.pallas_call(
        body,
        in_specs=[pl.BlockSpec(memory_space=pltpu.VMEM)] * (sets + len(operands) + len(so_far)),
        out_specs=[pl.BlockSpec(memory_space=pltpu.VMEM)] * sets,
        out_shape=[pltpu.VMEM((count, width), jnp.float32)] * sets,
        input_output_aliases=alias,
        cost_estimate=cost(
            2 * sets * count * 3 * width * hidden * len(shards), 6 * width * hidden * len(shards)
        ),
        compiler_params=pltpu.CompilerParams(vmem_limit_bytes=STEP_MIB * 2**20),
    )(*map(far, rows), *operands, *map(near, so_far))


def last_units(rows, gate, up):
    count, width = rows[0].shape
    hidden = gate.shape[1]

    def body(*refs):
        both = jnp.concatenate([refs[2][...], refs[3][...]], axis=1)
        for k in range(2):
            pre = times(refs[k][...], both)
            refs[4 + k][...] = gated(pre[:, :hidden], pre[:, hidden:])

    return pl.pallas_call(
        body,
        in_specs=[pl.BlockSpec(memory_space=pltpu.VMEM)] * 4,
        out_specs=[pl.BlockSpec(memory_space=pltpu.VMEM)] * 2,
        out_shape=[pltpu.VMEM((count, hidden), jnp.bfloat16)] * 2,
        cost_estimate=cost(8 * count * width * hidden, 4 * width * hidden),
        compiler_params=pltpu.CompilerParams(vmem_limit_bytes=STEP_MIB * 2**20),
        name="last_units",
    )(*map(far, rows), gate, up)


def last_down(units, down, so_far, dtype):
    count, width = so_far.shape

    def body(units_ref, down_ref, old_ref, new_ref):
        for at in range(0, width, CUT):
            added = times_t(units_ref[...], down_ref[at : at + CUT])
            new_ref[:, at : at + CUT] = (old_ref[:, at : at + CUT] + added).astype(dtype)

    return pl.pallas_call(
        body,
        in_specs=[pl.BlockSpec(memory_space=pltpu.VMEM)] * 3,
        out_specs=pl.BlockSpec(memory_space=pltpu.VMEM),
        out_shape=pltpu.VMEM((count, width), dtype),
        input_output_aliases={2: 0} if dtype == so_far.dtype else {},
        cost_estimate=cost(2 * count * width * units.shape[1], 8 * count * width),
        compiler_params=pltpu.CompilerParams(vmem_limit_bytes=STEP_MIB * 2**20),
        name="last_down",
    )(near(units), near(down), near(so_far))


def both_cores(mine, theirs):
    def body(mine_ref, theirs_ref, out_ref):
        out_ref[...] = (mine_ref[...] + theirs_ref[...].astype(jnp.float32)).astype(jnp.bfloat16)

    return pl.pallas_call(
        body,
        in_specs=[pl.BlockSpec(memory_space=pltpu.VMEM)] * 2,
        out_specs=pl.BlockSpec(memory_space=pltpu.VMEM),
        out_shape=pltpu.VMEM(mine.shape, jnp.bfloat16),
        cost_estimate=cost(mine.size, 8 * mine.size),
        compiler_params=pltpu.CompilerParams(vmem_limit_bytes=STEP_MIB * 2**20),
        name="both_cores",
    )(near(mine), near(theirs))


def z_ring(own):
    chips = lax.axis_size("tp") // 2
    fore, aft, found = own, own, []

    def moved(arrays, by):
        return [along_z(a, by) for a in arrays]

    for _ in range(1, chips // 2):
        fore, aft = moved(fore, 1), moved(aft, -1)
        found.append([fore, aft])
    return found, moved(fore, 1)


def expert_half(
    dispatched_group_activity,
    specialist_rmsgain,
    selected_specialist_ids,
    selected_specialist_share,
    specialist_switch_maps,
    specialist_widen_maps,
    specialist_shrink_maps,
):
    token_count, model_width = dispatched_group_activity.shape
    route_count = selected_specialist_ids.shape[1]
    expert_count = lax.axis_size("ep")
    slot_count = 3 * route_count * token_count // (2 * expert_count)
    own = [specialist_switch_maps[0], specialist_widen_maps[0], specialist_shrink_maps[0]]
    found, opposite = z_ring(own)
    outgoing, back = token_rows(
        dispatched_group_activity,
        specialist_rmsgain[None, :],
        selected_specialist_ids.T,
        selected_specialist_share.T,
        expert_count,
        slot_count,
    )

    def exchange(rows):
        blocks = rows.reshape(expert_count, slot_count, model_width)
        return lax.all_to_all(blocks, "ep", split_axis=0, concat_axis=0, tiled=True).reshape(
            expert_count * slot_count, model_width
        )

    kept = exchange(outgoing)
    lent = other_core(kept)
    found[0].append(own)
    partial = ()
    for shards in found:
        partial = expert_step((lent, kept), shards, tuple(partial))
    lent_units, kept_units = last_units((lent, kept), *opposite[:2])
    sent = last_down(lent_units, opposite[2], partial[0], jnp.bfloat16)
    given = other_core(sent)
    mine = last_down(kept_units, opposite[2], partial[1], jnp.float32)
    result = both_cores(mine, given)
    return weighted_sum(back, exchange(result))


def on_device(
    scan_source_values,
    switch_path_values,
    causal_filter_coefficients,
    scan_switch_blockmap,
    entry_switch_blockmap,
    feature_fading_speeds,
    spike_amount,
    final_linear_map,
    dispatched_group_activity,
    specialist_rmsgain,
    selected_specialist_ids,
    selected_specialist_share,
    specialist_switch_maps,
    specialist_widen_maps,
    specialist_shrink_maps,
):
    scan_path_result = mixer_half(
        scan_source_values,
        switch_path_values,
        causal_filter_coefficients,
        scan_switch_blockmap,
        entry_switch_blockmap,
        feature_fading_speeds,
        spike_amount,
        final_linear_map,
    )
    moe_out = expert_half(
        dispatched_group_activity,
        specialist_rmsgain,
        selected_specialist_ids,
        selected_specialist_share,
        specialist_switch_maps,
        specialist_widen_maps,
        specialist_shrink_maps,
    )
    return (scan_path_result, moe_out)


def solution(mesh):
    in_specs = (
        P("tp", "ep"),
        P("tp", "ep"),
        P(),
        P(),
        P(),
        P(),
        P("ep"),
        P(),
        P(("ep", "tp"), None),
        P(),
        P(("ep", "tp"), None),
        P(("ep", "tp"), None),
        P("ep", None, "tp"),
        P("ep", None, "tp"),
        P("ep", None, "tp"),
    )
    out_specs = (P(("ep", "tp"), None), P(("ep", "tp"), None))
    return jax.shard_map(
        lambda *args: on_device(*args), mesh=mesh, in_specs=in_specs, out_specs=out_specs, check_vma=False
    )
```

```python
import math

import jax
import jax.numpy as jnp
from jax import lax
from jax.experimental import pallas as pl
from jax.experimental.pallas import tpu as pltpu
from jax.sharding import PartitionSpec as P


LANES = 128
TILES_AT_ONCE = 4
CUT = 512
STEP_MIB = 12


def swapped(x, axis):
    return lax.all_to_all(x, axis, split_axis=0, concat_axis=0, tiled=True)


def from_behind(x, axis, by):
    count = lax.axis_size(axis)
    pairs = [(i, i + by) for i in range(count) if 0 <= i + by < count]
    return lax.ppermute(x, axis, pairs)


def along_z(x, by):
    tp = lax.axis_size("tp")
    return lax.ppermute(x, "tp", [(i, (i + (2 * by if i % 2 == 0 else -2 * by)) % tp) for i in range(tp)])


def other_core(x):
    tp = lax.axis_size("tp")
    return lax.ppermute(x, "tp", [(i, i ^ 1) for i in range(tp)])


def times(a, b):
    return jnp.dot(a, b, preferred_element_type=jnp.float32)


def times_t(a, b):
    return lax.dot_general(a, b, (((1,), (1,)), ((), ())), preferred_element_type=jnp.float32)


def far(x):
    return pltpu.with_memory_space_constraint(x, pltpu.HBM)


def cost(flops, moved):
    return pl.CostEstimate(flops=flops, bytes_accessed=moved, transcendentals=0)


def minus_expm1(v, exp_v):
    series = 1.0 + v * (1.0 / 9.0)
    for k in range(8, 1, -1):
        series = 1.0 + v * (1.0 / k) * series
    return jnp.where(v > -0.5, -v * series, 1.0 - exp_v)


def local_scan(x, halo, taps, rate_map, entry_map, fade, spike, group, blocks):
    channels, positions = x.shape
    block = rate_map.shape[1]

    def body(group_ref, x_ref, halo_ref, taps_ref, rate_ref, entry_ref, fade_ref, spike_ref, decay_ref, state_ref, total_ref, map_ref):
        map_ref[:block] = rate_ref[0].astype(jnp.float32).T.astype(jnp.bfloat16)
        map_ref[block:] = entry_ref[0].astype(jnp.float32).T.astype(jnp.bfloat16)
        lane = lax.broadcasted_iota(jnp.int32, (channels, LANES), 1)
        group = group_ref[0]
        per_row = LANES // channels

        def column(row):
            row = jnp.where(group % per_row == 0, row, pltpu.roll(row, LANES - channels, 1))
            return jnp.broadcast_to(row, (LANES, LANES)).T[:channels]

        at = pl.ds(pl.multiple_of(group // per_row * LANES, LANES), LANES)
        here = taps_ref[:, at].astype(jnp.float32)
        tap = [column(here[k : k + 1]) for k in range(4)]
        speed = -8.0 * column(fade_ref[pl.ds(group // per_row, 1), :])

        def rolled(a):
            return [pltpu.roll(a, s, 1) for s in (1, 2, 3)]

        def steps(chunk, carry):
            decay_run, state_run, before = carry[0], carry[1], list(carry[2:])
            found = []
            for t in range(TILES_AT_ONCE):
                at = pl.ds(pl.multiple_of((chunk * TILES_AT_ONCE + t) * LANES, LANES), LANES)
                here = x_ref[:, at].astype(jnp.float32)
                moved = rolled(here)
                conv = here * tap[3]
                for s in (1, 2, 3):
                    conv = conv + tap[3 - s] * jnp.where(lane < s, before[s - 1], moved[s - 1])
                before = moved
                conv = conv.astype(jnp.bfloat16)
                gates = times(map_ref[...], conv)
                rate = jax.nn.sigmoid(gates[:block])
                inflow = jax.nn.sigmoid(gates[block:])
                exponent = rate * speed + spike_ref[:, at]
                decay = jnp.exp(exponent)
                share = minus_expm1(2.0 * exponent, decay * decay)
                root = jnp.where(share > 0.0, jnp.sqrt(share), 0.0)
                state = root * inflow * conv.astype(jnp.float32)
                k = 1
                while k < LANES:
                    inside = lane >= k
                    state = state + jnp.where(inside, decay * pltpu.roll(state, k, 1), 0.0)
                    decay = decay * jnp.where(inside, pltpu.roll(decay, k, 1), 1.0)
                    k *= 2
                found.append((at, decay, state))
            for at, decay, state in found:
                state = state + decay * state_run
                decay = decay * decay_run
                decay_ref[:, at] = decay
                state_ref[:, at] = state
                decay_run = jnp.broadcast_to(decay[:, LANES - 1 :], decay.shape)
                state_run = jnp.broadcast_to(state[:, LANES - 1 :], state.shape)
            return (decay_run, state_run, *before)

        one = jnp.ones((channels, LANES), jnp.float32)
        first = (one, jnp.zeros_like(one), *rolled(halo_ref[...].astype(jnp.float32)))
        last = lax.fori_loop(0, positions // (LANES * TILES_AT_ONCE), steps, first)
        ends = jnp.where(lane == 0, last[0], jnp.where(lane == 1, last[1], 0.0))
        ends = jnp.concatenate([ends, jnp.zeros_like(ends)], axis=0).T[:8]
        total_ref[...] = jnp.broadcast_to(ends, total_ref.shape)

    whole = lambda *shape: pl.BlockSpec(shape, lambda i, g: (0,) * len(shape))
    return pl.pallas_call(
        body,
        grid_spec=pltpu.PrefetchScalarGridSpec(
            num_scalar_prefetch=1,
            grid=(1,),
            in_specs=[
                whole(channels, positions),
                whole(channels, LANES),
                whole(*taps.shape),
                pl.BlockSpec((1, block, block), lambda i, g: (g[0], 0, 0)),
                pl.BlockSpec((1, block, block), lambda i, g: (g[0], 0, 0)),
                whole(*fade.shape),
                whole(1, positions),
            ],
            out_specs=[
                whole(channels, positions),
                whole(channels, positions),
                whole(blocks, 8, LANES),
            ],
            scratch_shapes=[pltpu.VMEM((2 * block, block), jnp.bfloat16)],
        ),
        out_shape=[
            jax.ShapeDtypeStruct((channels, positions), jnp.float32),
            jax.ShapeDtypeStruct((channels, positions), jnp.float32),
            jax.ShapeDtypeStruct((blocks, 8, LANES), jnp.float32),
        ],
        cost_estimate=cost(4 * 10**9, 2 * 10**6),
        compiler_params=pltpu.CompilerParams(vmem_limit_bytes=12 * 2**20),
        name="local_scan",
    )(group, far(x), halo, far(taps), far(rate_map), far(entry_map), far(fade), far(spike))


def gated_states(decay, state, switch, totals, place, pieces):
    channels, positions = decay.shape
    width = positions // pieces

    def body(place_ref, decay_ref, state_ref, switch_ref, totals_ref, out_ref):
        entering = jnp.zeros((1, LANES), jnp.float32)
        for b in range(totals.shape[0]):
            passed = b < place_ref[0]
            entering = jnp.where(
                passed, totals_ref[b, 0:1] * entering + totals_ref[b, 1:2], entering
            )
        entering = jnp.broadcast_to(entering, (LANES, LANES)).T[:channels]
        for p in range(pieces):
            at = slice(p * width, (p + 1) * width)
            whole = state_ref[:, at] + decay_ref[:, at] * entering
            gate = jax.nn.gelu(switch_ref[:, at].astype(jnp.float32), approximate=True)
            out_ref[p] = (whole * gate).astype(jnp.bfloat16)

    vmem = pl.BlockSpec(memory_space=pltpu.VMEM)
    return pl.pallas_call(
        body,
        in_specs=[pl.BlockSpec(memory_space=pltpu.SMEM)] + [vmem] * 4,
        out_specs=vmem,
        out_shape=jax.ShapeDtypeStruct((pieces, channels, width), jnp.bfloat16),
        cost_estimate=cost(10**9, 2 * 10**6),
        compiler_params=pltpu.CompilerParams(vmem_limit_bytes=12 * 2**20),
        name="gated_states",
    )(place, decay, state, far(switch), totals)


def mixer_half(
    scan_source_values,
    switch_path_values,
    causal_filter_coefficients,
    scan_switch_blockmap,
    entry_switch_blockmap,
    feature_fading_speeds,
    spike_amount,
    final_linear_map,
):
    halo = from_behind(scan_source_values[:, -LANES:], "ep", 1)
    decay, state, total = local_scan(
        scan_source_values,
        halo,
        causal_filter_coefficients.T,
        scan_switch_blockmap,
        entry_switch_blockmap,
        feature_fading_speeds.reshape(-1, LANES),
        spike_amount[None, :],
        lax.axis_index("tp").astype(jnp.int32)[None],
        lax.axis_size("ep"),
    )
    pieces = gated_states(
        decay,
        state,
        switch_path_values,
        swapped(total, "ep"),
        lax.axis_index("ep").astype(jnp.int32)[None],
        lax.axis_size("tp"),
    )
    mixed = lax.all_to_all(pieces, "tp", split_axis=0, concat_axis=0, tiled=True)
    return lax.dot_general(
        mixed.reshape(-1, mixed.shape[2]),
        final_linear_map,
        (((0,), (0,)), ((), ())),
        preferred_element_type=jnp.float32,
    ).astype(jnp.bfloat16)


def token_rows(activity, gain, ids, share, slots, order):
    tokens, width = activity.shape
    experts = len(order)

    def body(act_ref, gain_ref, ids_ref, share_ref, rows_ref, back_ref):
        values = act_ref[...].astype(jnp.float32)
        scale = lax.rsqrt(jnp.mean(values * values, axis=1, keepdims=True) + 1e-06)
        normed = (values * scale * gain_ref[...].astype(jnp.float32)).astype(jnp.bfloat16)
        expert = lax.broadcasted_iota(jnp.int32, (experts, tokens), 0)
        earlier = lax.broadcasted_iota(jnp.int32, (tokens, tokens), 0)
        later = lax.broadcasted_iota(jnp.int32, (tokens, tokens), 1)
        ahead = (earlier < later).astype(jnp.float32).astype(jnp.bfloat16)
        slot = lax.broadcasted_iota(jnp.int32, (experts * slots, tokens), 0)
        count = jnp.zeros((experts, 1), jnp.float32)
        taken = jnp.zeros((experts * slots, tokens), jnp.float32)
        back = jnp.zeros((experts * slots, tokens), jnp.float32)
        for j in range(ids.shape[0]):
            mine = (expert == ids_ref[j : j + 1]).astype(jnp.float32)
            rank = times(mine.astype(jnp.bfloat16), ahead) + count
            rank = jnp.sum(mine * rank, axis=0, keepdims=True)
            count = count + jnp.sum(mine, axis=1, keepdims=True)
            chosen, rank = ids_ref[j : j + 1], rank.astype(jnp.int32)
            comes = jnp.zeros_like(chosen)
            for k, e in enumerate(order):
                comes = jnp.where(chosen == e, k, comes)
            taken = taken + jnp.where(slot == chosen * slots + rank, 1.0, 0.0)
            back = back + jnp.where(slot == comes * slots + rank, share_ref[j : j + 1], 0.0)
        rows_ref[...] = times(taken.astype(jnp.bfloat16), normed).astype(jnp.bfloat16)
        rest = back.T
        for k in range(3):
            part = rest.astype(jnp.bfloat16)
            back_ref[k] = part
            rest = rest - part.astype(jnp.float32)

    return pl.pallas_call(
        body,
        out_shape=[
            jax.ShapeDtypeStruct((experts * slots, width), jnp.bfloat16),
            jax.ShapeDtypeStruct((3, tokens, experts * slots), jnp.bfloat16),
        ],
        cost_estimate=cost(10**9, 2 * 10**6),
        compiler_params=pltpu.CompilerParams(vmem_limit_bytes=12 * 2**20),
        name="token_rows",
    )(far(activity), gain, far(ids), far(share))


def weighted_sum(back, results):
    parts, tokens, slots = back.shape
    width = results.shape[1]

    def body(back_ref, results_ref, out_ref):
        for at in range(0, width, CUT):
            cut = slice(at, at + CUT)
            each = times(back_ref[...], results_ref[:, cut])
            total = each[:tokens]
            for k in range(1, parts):
                total = total + each[k * tokens : (k + 1) * tokens]
            out_ref[:, cut] = total.astype(jnp.bfloat16)

    return pl.pallas_call(
        body,
        in_specs=[pl.BlockSpec(memory_space=pltpu.VMEM)] * 2,
        out_shape=jax.ShapeDtypeStruct((tokens, width), jnp.bfloat16),
        cost_estimate=cost(2 * parts * tokens * slots * width, 2 * slots * width),
        compiler_params=pltpu.CompilerParams(vmem_limit_bytes=12 * 2**20),
        name="weighted_sum",
    )(near(back.reshape(parts * tokens, slots)), near(results))


def near(x):
    return pltpu.with_memory_space_constraint(x, pltpu.VMEM)


def gated(gate_pre, up_pre):
    gate_cut = jnp.minimum(gate_pre, 7.0)
    up_cut = jnp.clip(up_pre, -7.0, 7.0)
    return ((up_cut + 1.0) * gate_cut * jax.nn.sigmoid(1.702 * gate_cut)).astype(jnp.bfloat16)


def expert_step(rows, shards, so_far, leaving=()):
    sets, count, width = len(rows), *rows[0].shape
    hidden = shards[0][0].shape[1]
    operands = [a for shard in shards for a in shard]
    layout = [(3 * k, 3 * k + 1, 3 * k + 2) for k in range(len(shards))]

    def body(*refs):
        row_refs, weights = refs[:sets], refs[sets : sets + len(operands)]
        refs = refs[sets + len(operands) :]
        old, new = (refs[:sets], refs[sets:]) if so_far else ((), refs)

        def side_by_side(ats):
            return jnp.concatenate([weights[at][...] for at in ats], axis=1)

        for k in range(sets):
            first = 0
            while first < len(shards):
                taken = layout[first : first + 2]
                base = old if first == 0 else new
                if len(taken) == 2:
                    gate_pre = times(row_refs[k][...], side_by_side([s[0] for s in taken]))
                    up_pre = times(row_refs[k][...], side_by_side([s[1] for s in taken]))
                else:
                    both = times(row_refs[k][...], side_by_side(taken[0][:2]))
                    gate_pre, up_pre = both[:, :hidden], both[:, hidden:]
                units = gated(gate_pre, up_pre)
                down = side_by_side([s[2] for s in taken])
                for at in range(0, width, CUT):
                    added = times_t(units, down[at : at + CUT])
                    if base:
                        added = base[k][:, at : at + CUT] + added
                    new[k][:, at : at + CUT] = added
                first += 2

    alias = {sets + len(operands) + k: k for k in range(len(so_far)) if k not in leaving}
    return pl.pallas_call(
        body,
        in_specs=[pl.BlockSpec(memory_space=pltpu.VMEM)] * (sets + len(operands) + len(so_far)),
        out_specs=[pl.BlockSpec(memory_space=pltpu.VMEM)] * sets,
        out_shape=[
            (jax.ShapeDtypeStruct if k in leaving else pltpu.VMEM)((count, width), jnp.float32)
            for k in range(sets)
        ],
        input_output_aliases=alias,
        cost_estimate=cost(
            2 * sets * count * 3 * width * hidden * len(shards), 6 * width * hidden * len(shards)
        ),
        compiler_params=pltpu.CompilerParams(vmem_limit_bytes=STEP_MIB * 2**20),
    )(*map(far, rows), *operands, *map(near, so_far))


def last_units(row, shards):
    count, width = row.shape
    hidden = shards[0][0].shape[1]

    def body(row_ref, *refs):
        weights, out_ref = refs[:-1], refs[-1]
        gate = jnp.concatenate([weights[0][...], weights[2][...]], axis=1)
        up = jnp.concatenate([weights[1][...], weights[3][...]], axis=1)
        out_ref[...] = gated(times(row_ref[...], gate), times(row_ref[...], up))

    return pl.pallas_call(
        body,
        in_specs=[pl.BlockSpec(memory_space=pltpu.VMEM)] * 5,
        out_specs=pl.BlockSpec(memory_space=pltpu.VMEM),
        out_shape=pltpu.VMEM((count, 2 * hidden), jnp.bfloat16),
        cost_estimate=cost(8 * count * width * hidden, 8 * width * hidden),
        compiler_params=pltpu.CompilerParams(vmem_limit_bytes=STEP_MIB * 2**20),
        name="last_units",
    )(row, *(a for shard in shards for a in shard))


def joined(mine, given):
    def body(mine_ref, given_ref, out_ref):
        out_ref[...] = mine_ref[...] + given_ref[...]

    return pl.pallas_call(
        body,
        in_specs=[pl.BlockSpec(memory_space=pltpu.VMEM)] * 2,
        out_specs=pl.BlockSpec(memory_space=pltpu.VMEM),
        out_shape=pltpu.VMEM(mine.shape, mine.dtype),
        input_output_aliases={0: 0},
        cost_estimate=cost(mine.size, 12 * mine.size),
        compiler_params=pltpu.CompilerParams(vmem_limit_bytes=STEP_MIB * 2**20),
        name="joined",
    )(near(mine), given)


def last_down(units, part, down, so_far, order, dtype):
    count, width = so_far.shape
    hidden = down.shape[1]
    rows = count // len(order)

    def body(units_ref, down_ref, old_ref, new_ref):
        mine = units_ref[:, part * hidden : (part + 1) * hidden]
        for at in range(0, width, CUT):
            cut = slice(at, at + CUT)
            total = (old_ref[:, cut] + times_t(mine, down_ref[cut])).astype(dtype)
            for k, place in enumerate(order):
                new_ref[k * rows : (k + 1) * rows, cut] = total[place * rows : (place + 1) * rows]

    operands = (units, down, so_far)
    return pl.pallas_call(
        body,
        in_specs=[pl.BlockSpec(memory_space=pltpu.VMEM)] * len(operands),
        out_specs=pl.BlockSpec(memory_space=pltpu.VMEM),
        out_shape=pltpu.VMEM((count, width), dtype),
        input_output_aliases={2: 0} if dtype == so_far.dtype else {},
        cost_estimate=cost(2 * count * width * hidden, 8 * count * width),
        compiler_params=pltpu.CompilerParams(vmem_limit_bytes=STEP_MIB * 2**20),
        name="last_down",
    )(*map(near, operands))


def z_ring(own):
    chips = lax.axis_size("tp") // 2
    fore, aft, found = own, own, []

    def moved(arrays, by):
        return [along_z(a, by) for a in arrays]

    for _ in range(1, chips // 2):
        fore, aft = moved(fore, 1), moved(aft, -1)
        found.append([fore, aft])
    return found, moved(fore, 1)


def interleaved(count):
    side = math.isqrt(count)
    key = lambda i: sum(
        ((i % side >> b & 1) << 2 * b) | ((i // side >> b & 1) << 2 * b + 1) for b in range(side)
    )
    return sorted(range(count), key=key)


def expert_half(
    dispatched_group_activity,
    specialist_rmsgain,
    selected_specialist_ids,
    selected_specialist_share,
    specialist_switch_maps,
    specialist_widen_maps,
    specialist_shrink_maps,
):
    token_count, model_width = dispatched_group_activity.shape
    route_count = selected_specialist_ids.shape[1]
    expert_count = lax.axis_size("ep")
    slot_count = 3 * route_count * token_count // (2 * expert_count)
    own = [specialist_switch_maps[0], specialist_widen_maps[0], specialist_shrink_maps[0]]
    found, opposite = z_ring(own)
    order = interleaved(expert_count)
    outgoing, back = token_rows(
        dispatched_group_activity,
        specialist_rmsgain[None, :],
        selected_specialist_ids.T,
        selected_specialist_share.T,
        slot_count,
        order,
    )

    def exchange(rows):
        blocks = rows.reshape(expert_count, slot_count, model_width)
        return lax.all_to_all(blocks, "ep", split_axis=0, concat_axis=0, tiled=True).reshape(
            expert_count * slot_count, model_width
        )

    kept = exchange(outgoing)
    lent = other_core(kept)
    found[0].append(own)
    partial = ()
    for r, shards in enumerate(found):
        leaving = (0,) if r + 1 == len(found) else ()
        partial = expert_step((lent, kept), shards, tuple(partial), leaving)
    given = other_core(partial[0])
    theirs = [other_core(a) for a in opposite]
    units = last_units(kept, [opposite[:2], theirs[:2]])
    mine = joined(partial[1], given)
    mine = last_down(units, 0, opposite[2], mine, (0,), jnp.float32)
    result = last_down(units, 1, theirs[2], mine, order, jnp.bfloat16)
    returned = lax.all_to_all(
        result.reshape(expert_count, slot_count, model_width),
        "ep",
        split_axis=0,
        concat_axis=0,
        tiled=True,
        axis_index_groups=[order],
    ).reshape(expert_count * slot_count, model_width)
    return weighted_sum(back, returned)


def on_device(
    scan_source_values,
    switch_path_values,
    causal_filter_coefficients,
    scan_switch_blockmap,
    entry_switch_blockmap,
    feature_fading_speeds,
    spike_amount,
    final_linear_map,
    dispatched_group_activity,
    specialist_rmsgain,
    selected_specialist_ids,
    selected_specialist_share,
    specialist_switch_maps,
    specialist_widen_maps,
    specialist_shrink_maps,
):
    scan_path_result = mixer_half(
        scan_source_values,
        switch_path_values,
        causal_filter_coefficients,
        scan_switch_blockmap,
        entry_switch_blockmap,
        feature_fading_speeds,
        spike_amount,
        final_linear_map,
    )
    moe_out = expert_half(
        dispatched_group_activity,
        specialist_rmsgain,
        selected_specialist_ids,
        selected_specialist_share,
        specialist_switch_maps,
        specialist_widen_maps,
        specialist_shrink_maps,
    )
    return (scan_path_result, moe_out)


def solution(mesh):
    in_specs = (
        P("tp", "ep"),
        P("tp", "ep"),
        P(),
        P(),
        P(),
        P(),
        P("ep"),
        P(),
        P(("ep", "tp"), None),
        P(),
        P(("ep", "tp"), None),
        P(("ep", "tp"), None),
        P("ep", None, "tp"),
        P("ep", None, "tp"),
        P("ep", None, "tp"),
    )
    out_specs = (P(("ep", "tp"), None), P(("ep", "tp"), None))
    return jax.shard_map(
        lambda *args: on_device(*args), mesh=mesh, in_specs=in_specs, out_specs=out_specs, check_vma=False
    )
```

```python
import math

import jax
import jax.numpy as jnp
from jax import lax
from jax.experimental import pallas as pl
from jax.experimental.pallas import tpu as pltpu
from jax.sharding import PartitionSpec as P


LANES = 128
TILES_AT_ONCE = 4
CUT = 512
STEP_MIB = 12
SHARE_TERMS = 2


def swapped(x, axis):
    return lax.all_to_all(x, axis, split_axis=0, concat_axis=0, tiled=True)


def from_behind(x, axis, by):
    count = lax.axis_size(axis)
    pairs = [(i, i + by) for i in range(count) if 0 <= i + by < count]
    return lax.ppermute(x, axis, pairs)


def along_z(x, by):
    tp = lax.axis_size("tp")
    return lax.ppermute(x, "tp", [(i, (i + (2 * by if i % 2 == 0 else -2 * by)) % tp) for i in range(tp)])


def other_core(x):
    tp = lax.axis_size("tp")
    return lax.ppermute(x, "tp", [(i, i ^ 1) for i in range(tp)])


def times(a, b):
    return jnp.dot(a, b, preferred_element_type=jnp.float32)


def times_t(a, b):
    return lax.dot_general(a, b, (((1,), (1,)), ((), ())), preferred_element_type=jnp.float32)


def far(x):
    return pltpu.with_memory_space_constraint(x, pltpu.HBM)


def cost(flops, moved):
    return pl.CostEstimate(flops=flops, bytes_accessed=moved, transcendentals=0)


def minus_expm1(v, exp_v):
    series = 1.0 + v * (1.0 / 9.0)
    for k in range(8, 1, -1):
        series = 1.0 + v * (1.0 / k) * series
    return jnp.where(v > -0.5, -v * series, 1.0 - exp_v)


def local_scan(x, halo, taps, rate_map, entry_map, fade, spike, group, blocks):
    channels, positions = x.shape
    block = rate_map.shape[1]

    def body(group_ref, x_ref, halo_ref, taps_ref, rate_ref, entry_ref, fade_ref, spike_ref, decay_ref, state_ref, total_ref, map_ref):
        map_ref[:block] = rate_ref[0].astype(jnp.float32).T.astype(jnp.bfloat16)
        map_ref[block:] = entry_ref[0].astype(jnp.float32).T.astype(jnp.bfloat16)
        lane = lax.broadcasted_iota(jnp.int32, (channels, LANES), 1)
        group = group_ref[0]
        per_row = LANES // channels

        def column(row):
            row = jnp.where(group % per_row == 0, row, pltpu.roll(row, LANES - channels, 1))
            return jnp.broadcast_to(row, (LANES, LANES)).T[:channels]

        at = pl.ds(pl.multiple_of(group // per_row * LANES, LANES), LANES)
        here = taps_ref[:, at].astype(jnp.float32)
        tap = [column(here[k : k + 1]) for k in range(4)]
        speed = -8.0 * column(fade_ref[pl.ds(group // per_row, 1), :])

        def rolled(a):
            return [pltpu.roll(a, s, 1) for s in (1, 2, 3)]

        def steps(chunk, carry):
            decay_run, state_run, before = carry[0], carry[1], list(carry[2:])
            found = []
            for t in range(TILES_AT_ONCE):
                at = pl.ds(pl.multiple_of((chunk * TILES_AT_ONCE + t) * LANES, LANES), LANES)
                here = x_ref[:, at].astype(jnp.float32)
                moved = rolled(here)
                conv = here * tap[3]
                for s in (1, 2, 3):
                    conv = conv + tap[3 - s] * jnp.where(lane < s, before[s - 1], moved[s - 1])
                before = moved
                conv = conv.astype(jnp.bfloat16)
                gates = times(map_ref[...], conv)
                rate = jax.nn.sigmoid(gates[:block])
                inflow = jax.nn.sigmoid(gates[block:])
                exponent = rate * speed + spike_ref[:, at]
                decay = jnp.exp(exponent)
                share = minus_expm1(2.0 * exponent, decay * decay)
                root = jnp.where(share > 0.0, jnp.sqrt(share), 0.0)
                state = root * inflow * conv.astype(jnp.float32)
                k = 1
                while k < LANES:
                    inside = lane >= k
                    state = state + jnp.where(inside, decay * pltpu.roll(state, k, 1), 0.0)
                    decay = decay * jnp.where(inside, pltpu.roll(decay, k, 1), 1.0)
                    k *= 2
                found.append((at, decay, state))
            for at, decay, state in found:
                state = state + decay * state_run
                decay = decay * decay_run
                decay_ref[:, at] = decay
                state_ref[:, at] = state
                decay_run = jnp.broadcast_to(decay[:, LANES - 1 :], decay.shape)
                state_run = jnp.broadcast_to(state[:, LANES - 1 :], state.shape)
            return (decay_run, state_run, *before)

        one = jnp.ones((channels, LANES), jnp.float32)
        first = (one, jnp.zeros_like(one), *rolled(halo_ref[...].astype(jnp.float32)))
        last = lax.fori_loop(0, positions // (LANES * TILES_AT_ONCE), steps, first)
        ends = jnp.where(lane == 0, last[0], jnp.where(lane == 1, last[1], 0.0))
        ends = jnp.concatenate([ends, jnp.zeros_like(ends)], axis=0).T[:8]
        total_ref[...] = jnp.broadcast_to(ends, total_ref.shape)

    whole = lambda *shape: pl.BlockSpec(shape, lambda i, g: (0,) * len(shape))
    return pl.pallas_call(
        body,
        grid_spec=pltpu.PrefetchScalarGridSpec(
            num_scalar_prefetch=1,
            grid=(1,),
            in_specs=[
                whole(channels, positions),
                whole(channels, LANES),
                whole(*taps.shape),
                pl.BlockSpec((1, block, block), lambda i, g: (g[0], 0, 0)),
                pl.BlockSpec((1, block, block), lambda i, g: (g[0], 0, 0)),
                whole(*fade.shape),
                whole(1, positions),
            ],
            out_specs=[
                whole(channels, positions),
                whole(channels, positions),
                whole(blocks, 8, LANES),
            ],
            scratch_shapes=[pltpu.VMEM((2 * block, block), jnp.bfloat16)],
        ),
        out_shape=[
            jax.ShapeDtypeStruct((channels, positions), jnp.float32),
            jax.ShapeDtypeStruct((channels, positions), jnp.float32),
            jax.ShapeDtypeStruct((blocks, 8, LANES), jnp.float32),
        ],
        cost_estimate=cost(4 * 10**9, 2 * 10**6),
        compiler_params=pltpu.CompilerParams(vmem_limit_bytes=12 * 2**20),
        name="local_scan",
    )(group, far(x), halo, far(taps), far(rate_map), far(entry_map), far(fade), far(spike))


def gated_states(decay, state, switch, totals, place, pieces):
    channels, positions = decay.shape
    width = positions // pieces

    def body(place_ref, decay_ref, state_ref, switch_ref, totals_ref, out_ref):
        entering = jnp.zeros((1, LANES), jnp.float32)
        for b in range(totals.shape[0]):
            passed = b < place_ref[0]
            entering = jnp.where(
                passed, totals_ref[b, 0:1] * entering + totals_ref[b, 1:2], entering
            )
        entering = jnp.broadcast_to(entering, (LANES, LANES)).T[:channels]
        for p in range(pieces):
            at = slice(p * width, (p + 1) * width)
            whole = state_ref[:, at] + decay_ref[:, at] * entering
            gate = jax.nn.gelu(switch_ref[:, at].astype(jnp.float32), approximate=True)
            out_ref[p] = (whole * gate).astype(jnp.bfloat16)

    vmem = pl.BlockSpec(memory_space=pltpu.VMEM)
    return pl.pallas_call(
        body,
        in_specs=[pl.BlockSpec(memory_space=pltpu.SMEM)] + [vmem] * 4,
        out_specs=vmem,
        out_shape=jax.ShapeDtypeStruct((pieces, channels, width), jnp.bfloat16),
        cost_estimate=cost(10**9, 2 * 10**6),
        compiler_params=pltpu.CompilerParams(vmem_limit_bytes=12 * 2**20),
        name="gated_states",
    )(place, decay, state, far(switch), totals)


def mixer_half(
    scan_source_values,
    switch_path_values,
    causal_filter_coefficients,
    scan_switch_blockmap,
    entry_switch_blockmap,
    feature_fading_speeds,
    spike_amount,
    final_linear_map,
):
    halo = from_behind(scan_source_values[:, -LANES:], "ep", 1)
    decay, state, total = local_scan(
        scan_source_values,
        halo,
        causal_filter_coefficients.T,
        scan_switch_blockmap,
        entry_switch_blockmap,
        feature_fading_speeds.reshape(-1, LANES),
        spike_amount[None, :],
        lax.axis_index("tp").astype(jnp.int32)[None],
        lax.axis_size("ep"),
    )
    pieces = gated_states(
        decay,
        state,
        switch_path_values,
        swapped(total, "ep"),
        lax.axis_index("ep").astype(jnp.int32)[None],
        lax.axis_size("tp"),
    )
    mixed = lax.all_to_all(pieces, "tp", split_axis=0, concat_axis=0, tiled=True)
    return lax.dot_general(
        mixed.reshape(-1, mixed.shape[2]),
        final_linear_map,
        (((0,), (0,)), ((), ())),
        preferred_element_type=jnp.float32,
    ).astype(jnp.bfloat16)


def token_rows(activity, gain, ids, share, slots, order):
    tokens, width = activity.shape
    experts = len(order)

    def body(act_ref, gain_ref, ids_ref, share_ref, rows_ref, back_ref):
        values = act_ref[...].astype(jnp.float32)
        scale = lax.rsqrt(jnp.mean(values * values, axis=1, keepdims=True) + 1e-06)
        normed = (values * scale * gain_ref[...].astype(jnp.float32)).astype(jnp.bfloat16)
        expert = lax.broadcasted_iota(jnp.int32, (experts, tokens), 0)
        earlier = lax.broadcasted_iota(jnp.int32, (tokens, tokens), 0)
        later = lax.broadcasted_iota(jnp.int32, (tokens, tokens), 1)
        ahead = (earlier < later).astype(jnp.float32).astype(jnp.bfloat16)
        slot = lax.broadcasted_iota(jnp.int32, (experts * slots, tokens), 0)
        count = jnp.zeros((experts, 1), jnp.float32)
        taken = jnp.zeros((experts * slots, tokens), jnp.float32)
        back = jnp.zeros((experts * slots, tokens), jnp.float32)
        for j in range(ids.shape[0]):
            mine = (expert == ids_ref[j : j + 1]).astype(jnp.float32)
            rank = times(mine.astype(jnp.bfloat16), ahead) + count
            rank = jnp.sum(mine * rank, axis=0, keepdims=True)
            count = count + jnp.sum(mine, axis=1, keepdims=True)
            chosen, rank = ids_ref[j : j + 1], rank.astype(jnp.int32)
            comes = jnp.zeros_like(chosen)
            for k, e in enumerate(order):
                comes = jnp.where(chosen == e, k, comes)
            taken = taken + jnp.where(slot == chosen * slots + rank, 1.0, 0.0)
            back = back + jnp.where(slot == comes * slots + rank, share_ref[j : j + 1], 0.0)
        rows_ref[...] = times(taken.astype(jnp.bfloat16), normed).astype(jnp.bfloat16)
        rest = back.T
        for k in range(SHARE_TERMS):
            part = rest.astype(jnp.bfloat16)
            back_ref[k] = part
            rest = rest - part.astype(jnp.float32)

    return pl.pallas_call(
        body,
        out_shape=[
            jax.ShapeDtypeStruct((experts * slots, width), jnp.bfloat16),
            jax.ShapeDtypeStruct((SHARE_TERMS, tokens, experts * slots), jnp.bfloat16),
        ],
        cost_estimate=cost(10**9, 2 * 10**6),
        compiler_params=pltpu.CompilerParams(vmem_limit_bytes=12 * 2**20),
        name="token_rows",
    )(far(activity), gain, far(ids), far(share))


def weighted_sum(back, results):
    parts, tokens, slots = back.shape
    width = results.shape[1]

    def body(back_ref, results_ref, out_ref, done_ref, sems):
        copies = []
        for k, at in enumerate(range(0, width, CUT)):
            cut = slice(at, at + CUT)
            each = times(back_ref[...], results_ref[:, cut])
            total = each[:tokens]
            for p in range(1, parts):
                total = total + each[p * tokens : (p + 1) * tokens]
            done_ref[:, cut] = total.astype(jnp.bfloat16)
            copies.append(
                pltpu.make_async_copy(done_ref.at[:, cut], out_ref.at[:, cut], sems.at[k])
            )
            copies[-1].start()
        for copy in copies:
            copy.wait()

    return pl.pallas_call(
        body,
        in_specs=[pl.BlockSpec(memory_space=pltpu.VMEM)] * 2,
        out_specs=pl.BlockSpec(memory_space=pl.ANY),
        out_shape=jax.ShapeDtypeStruct((tokens, width), jnp.bfloat16),
        scratch_shapes=[
            pltpu.VMEM((tokens, width), jnp.bfloat16),
            pltpu.SemaphoreType.DMA((width // CUT,)),
        ],
        cost_estimate=cost(2 * parts * tokens * slots * width, 2 * slots * width),
        compiler_params=pltpu.CompilerParams(vmem_limit_bytes=12 * 2**20),
        name="weighted_sum",
    )(near(back.reshape(parts * tokens, slots)), near(results))


def near(x):
    return pltpu.with_memory_space_constraint(x, pltpu.VMEM)


def gated(gate_pre, up_pre):
    gate_cut = jnp.minimum(gate_pre, 7.0)
    up_cut = jnp.clip(up_pre, -7.0, 7.0)
    return ((up_cut + 1.0) * gate_cut * jax.nn.sigmoid(1.702 * gate_cut)).astype(jnp.bfloat16)


def expert_step(rows, shards, so_far, leaving=()):
    sets, count, width = len(rows), *rows[0].shape
    hidden = shards[0][0].shape[1]
    operands = [a for shard in shards for a in shard]
    layout = [(3 * k, 3 * k + 1, 3 * k + 2) for k in range(len(shards))]

    def body(*refs):
        row_refs, weights = refs[:sets], refs[sets : sets + len(operands)]
        refs = refs[sets + len(operands) :]
        old, new = (refs[:sets], refs[sets:]) if so_far else ((), refs)

        def side_by_side(ats):
            return jnp.concatenate([weights[at][...] for at in ats], axis=1)

        for k in range(sets):
            first = 0
            while first < len(shards):
                taken = layout[first : first + 2]
                base = old if first == 0 else new
                if len(taken) == 2:
                    gate_pre = times(row_refs[k][...], side_by_side([s[0] for s in taken]))
                    up_pre = times(row_refs[k][...], side_by_side([s[1] for s in taken]))
                else:
                    both = times(row_refs[k][...], side_by_side(taken[0][:2]))
                    gate_pre, up_pre = both[:, :hidden], both[:, hidden:]
                units = gated(gate_pre, up_pre)
                down = side_by_side([s[2] for s in taken])
                for at in range(0, width, CUT):
                    added = times_t(units, down[at : at + CUT])
                    if base:
                        added = base[k][:, at : at + CUT] + added
                    new[k][:, at : at + CUT] = added
                first += 2

    alias = {sets + len(operands) + k: k for k in range(len(so_far)) if k not in leaving}
    return pl.pallas_call(
        body,
        in_specs=[pl.BlockSpec(memory_space=pltpu.VMEM)] * (sets + len(operands) + len(so_far)),
        out_specs=[pl.BlockSpec(memory_space=pltpu.VMEM)] * sets,
        out_shape=[
            (jax.ShapeDtypeStruct if k in leaving else pltpu.VMEM)((count, width), jnp.float32)
            for k in range(sets)
        ],
        input_output_aliases=alias,
        cost_estimate=cost(
            2 * sets * count * 3 * width * hidden * len(shards), 6 * width * hidden * len(shards)
        ),
        compiler_params=pltpu.CompilerParams(vmem_limit_bytes=STEP_MIB * 2**20),
    )(*map(far, rows), *operands, *map(near, so_far))


def last_units(row, shards):
    count, width = row.shape
    hidden = shards[0][0].shape[1]

    def body(row_ref, *refs):
        weights, out_ref = refs[:-1], refs[-1]
        gate = jnp.concatenate([weights[0][...], weights[2][...]], axis=1)
        up = jnp.concatenate([weights[1][...], weights[3][...]], axis=1)
        out_ref[...] = gated(times(row_ref[...], gate), times(row_ref[...], up))

    return pl.pallas_call(
        body,
        in_specs=[pl.BlockSpec(memory_space=pltpu.VMEM)] * 5,
        out_specs=pl.BlockSpec(memory_space=pltpu.VMEM),
        out_shape=pltpu.VMEM((count, 2 * hidden), jnp.bfloat16),
        cost_estimate=cost(8 * count * width * hidden, 8 * width * hidden),
        compiler_params=pltpu.CompilerParams(vmem_limit_bytes=STEP_MIB * 2**20),
        name="last_units",
    )(row, *(a for shard in shards for a in shard))


def joined(mine, given):
    def body(mine_ref, given_ref, out_ref):
        out_ref[...] = mine_ref[...] + given_ref[...]

    return pl.pallas_call(
        body,
        in_specs=[pl.BlockSpec(memory_space=pltpu.VMEM)] * 2,
        out_specs=pl.BlockSpec(memory_space=pltpu.VMEM),
        out_shape=pltpu.VMEM(mine.shape, mine.dtype),
        input_output_aliases={0: 0},
        cost_estimate=cost(mine.size, 12 * mine.size),
        compiler_params=pltpu.CompilerParams(vmem_limit_bytes=STEP_MIB * 2**20),
        name="joined",
    )(near(mine), given)


def last_down(units, part, down, so_far, order, dtype):
    count, width = so_far.shape
    hidden = down.shape[1]
    rows = count // len(order)

    def body(units_ref, down_ref, old_ref, new_ref):
        mine = units_ref[:, part * hidden : (part + 1) * hidden]
        for at in range(0, width, CUT):
            cut = slice(at, at + CUT)
            total = (old_ref[:, cut] + times_t(mine, down_ref[cut])).astype(dtype)
            for k, place in enumerate(order):
                new_ref[k * rows : (k + 1) * rows, cut] = total[place * rows : (place + 1) * rows]

    operands = (units, down, so_far)
    return pl.pallas_call(
        body,
        in_specs=[pl.BlockSpec(memory_space=pltpu.VMEM)] * len(operands),
        out_specs=pl.BlockSpec(memory_space=pltpu.VMEM),
        out_shape=pltpu.VMEM((count, width), dtype),
        input_output_aliases={2: 0} if dtype == so_far.dtype else {},
        cost_estimate=cost(2 * count * width * hidden, 8 * count * width),
        compiler_params=pltpu.CompilerParams(vmem_limit_bytes=STEP_MIB * 2**20),
        name="last_down",
    )(*map(near, operands))


def z_ring(own):
    chips = lax.axis_size("tp") // 2
    fore, aft, found = own, own, []

    def moved(arrays, by):
        return [along_z(a, by) for a in arrays]

    for _ in range(1, chips // 2):
        fore, aft = moved(fore, 1), moved(aft, -1)
        found.append([fore, aft])
    return found, moved(fore, 1)


def interleaved(count):
    side = math.isqrt(count)
    key = lambda i: sum(
        ((i % side >> b & 1) << 2 * b) | ((i // side >> b & 1) << 2 * b + 1) for b in range(side)
    )
    return sorted(range(count), key=key)


def expert_half(
    dispatched_group_activity,
    specialist_rmsgain,
    selected_specialist_ids,
    selected_specialist_share,
    specialist_switch_maps,
    specialist_widen_maps,
    specialist_shrink_maps,
):
    token_count, model_width = dispatched_group_activity.shape
    route_count = selected_specialist_ids.shape[1]
    expert_count = lax.axis_size("ep")
    slot_count = 3 * route_count * token_count // (2 * expert_count)
    own = [specialist_switch_maps[0], specialist_widen_maps[0], specialist_shrink_maps[0]]
    found, opposite = z_ring(own)
    order = interleaved(expert_count)
    outgoing, back = token_rows(
        dispatched_group_activity,
        specialist_rmsgain[None, :],
        selected_specialist_ids.T,
        selected_specialist_share.T,
        slot_count,
        order,
    )

    def exchange(rows):
        blocks = rows.reshape(expert_count, slot_count, model_width)
        return lax.all_to_all(blocks, "ep", split_axis=0, concat_axis=0, tiled=True).reshape(
            expert_count * slot_count, model_width
        )

    kept = exchange(outgoing)
    lent = other_core(kept)
    found[0].append(own)
    partial = ()
    for r, shards in enumerate(found):
        leaving = (0,) if r + 1 == len(found) else ()
        partial = expert_step((lent, kept), shards, tuple(partial), leaving)
    given = other_core(partial[0])
    theirs = [other_core(a) for a in opposite]
    units = last_units(kept, [opposite[:2], theirs[:2]])
    mine = joined(partial[1], given)
    mine = last_down(units, 0, opposite[2], mine, (0,), jnp.float32)
    result = last_down(units, 1, theirs[2], mine, order, jnp.bfloat16)
    returned = lax.all_to_all(
        result.reshape(expert_count, slot_count, model_width),
        "ep",
        split_axis=0,
        concat_axis=0,
        tiled=True,
        axis_index_groups=[order],
    ).reshape(expert_count * slot_count, model_width)
    return weighted_sum(back, returned)


def on_device(
    scan_source_values,
    switch_path_values,
    causal_filter_coefficients,
    scan_switch_blockmap,
    entry_switch_blockmap,
    feature_fading_speeds,
    spike_amount,
    final_linear_map,
    dispatched_group_activity,
    specialist_rmsgain,
    selected_specialist_ids,
    selected_specialist_share,
    specialist_switch_maps,
    specialist_widen_maps,
    specialist_shrink_maps,
):
    scan_path_result = mixer_half(
        scan_source_values,
        switch_path_values,
        causal_filter_coefficients,
        scan_switch_blockmap,
        entry_switch_blockmap,
        feature_fading_speeds,
        spike_amount,
        final_linear_map,
    )
    moe_out = expert_half(
        dispatched_group_activity,
        specialist_rmsgain,
        selected_specialist_ids,
        selected_specialist_share,
        specialist_switch_maps,
        specialist_widen_maps,
        specialist_shrink_maps,
    )
    return (scan_path_result, moe_out)


def solution(mesh):
    in_specs = (
        P("tp", "ep"),
        P("tp", "ep"),
        P(),
        P(),
        P(),
        P(),
        P("ep"),
        P(),
        P(("ep", "tp"), None),
        P(),
        P(("ep", "tp"), None),
        P(("ep", "tp"), None),
        P("ep", None, "tp"),
        P("ep", None, "tp"),
        P("ep", None, "tp"),
    )
    out_specs = (P(("ep", "tp"), None), P(("ep", "tp"), None))
    return jax.shard_map(
        lambda *args: on_device(*args), mesh=mesh, in_specs=in_specs, out_specs=out_specs, check_vma=False
    )
```
